512 devices in a mesh: rep: 2 (over z_hi), fs: 32 (over z_lo, y), tp: 8 (over x, core).
Axes of the slice: x: 4, y: 4, z: 16 (z_hi: 2, z_lo: 8; z = z_hi * 8 + z_lo), core: 2. Of those that a mesh axis runs over, the one named last changes fastest.
Arguments:
- tokens: bfloat16 [32768, 2048], P(('rep', 'fs')), may hold values from -6 to 6
- recurrence_branch_weight: bfloat16 [2048, 2048], P('fs', 'tp'), may hold values from -0.125 to 0.125
- gate_branch_weight: bfloat16 [2048, 2048], P('fs', 'tp'), may hold values from -0.125 to 0.125
- convolution_kernel: bfloat16 [4, 2048], P(None, 'tp'), may hold values from -3 to 3
- recurrence_gate_blockwise: bfloat16 [8, 256, 256], P('tp'), may hold values from -0.375 to 0.375
- input_gate_blockwise: bfloat16 [8, 256, 256], P('tp'), may hold values from -0.375 to 0.375
- channel_decay_param: float32 [2048], P('tp')
- token_decay_shift: float32 [32768, 2048], P(('rep', 'fs'), 'tp'), may hold values from -1 to 0
- recurrence_output_weight: bfloat16 [2048, 2048], P('tp', 'fs'), may hold values from -0.5 to 0.5
- first_norm_gain: float32 [2048], replicated, may hold values from 0.1 to 1.9
- feedforward_gate_weight: bfloat16 [2048, 5120], P('fs', 'tp'), may hold values from -0.125 to 0.125
- feedforward_up_weight: bfloat16 [2048, 5120], P('fs', 'tp'), may hold values from -0.125 to 0.125
- feedforward_down_weight: bfloat16 [5120, 2048], P('tp', 'fs'), may hold values from -0.15625 to 0.15625
- second_norm_gain: float32 [2048], replicated, may hold values from 0.1 to 1.9
Outputs:
- layer_out: bfloat16 [32768, 2048], P(('rep', 'fs', 'tp'))
The draws below stay inside these ranges and needn't reach their ends.
All inputs are finite; a program needn't handle non-finite values.
Results may differ from the reference program's by a relative error of at most 0.02.
Values may be sent and summed in bfloat16 or wider, within the bound.
No kernel may reach another device: no remote copies, remote signals or barrier semaphores. Data moves between devices by JAX's collectives and lax.ppermute only.
A program may use at most 64 MiB of HBM per device.

```python
import math
import jax
import jax.numpy as jnp
from jax import lax

MODEL_WIDTH = 2048
FF = 5120
LRU_BLOCKS = 8
BLOCK = 256
CONV = 4
SEQUENCE_TOKENS = 512
RECURRENT_WIDTH = 2048
ROWS_ALL = 32768
N_TP = 8


def draw_channel_decay_param(key, part):
    key_flag = jax.random.fold_in(key, 11)
    key_slow = jax.random.fold_in(key, 12)
    key_fast = jax.random.fold_in(key, 13)
    quick = jax.random.randint(key_flag, (RECURRENT_WIDTH,), 0, 2) == 1
    slow_value = math.log(4.0 * SEQUENCE_TOKENS) + jax.random.uniform(key_slow, (RECURRENT_WIDTH,), jnp.float32, 0.0, 1.5)
    fast_value = math.log(4.0 * min(50.0, SEQUENCE_TOKENS / 4.0)) + jax.random.uniform(key_fast, (RECURRENT_WIDTH,), jnp.float32, -0.5, 0.5)
    return jnp.where(quick, fast_value, slow_value).astype(jnp.float32)


def draw_token_decay_shift(key, part):
    key_where = jax.random.fold_in(key, 21)
    key_depth = jax.random.fold_in(key, 22)
    struck = jax.random.randint(key_where, (ROWS_ALL, 1), 0, SEQUENCE_TOKENS) < 3
    depth = jax.random.uniform(key_depth, (ROWS_ALL, RECURRENT_WIDTH), jnp.float32, 0.22, 0.69)
    return jnp.where(struck, -depth, 0.0).astype(jnp.float32)


def block_levels(key, extent, cuts, low, top_value):
    level = 1.0
    for axis_at, parts in cuts:
        heights = jax.random.uniform(jax.random.fold_in(jax.random.fold_in(key, 6), axis_at), (parts,), jnp.float32, low / len(cuts), top_value / len(cuts))
        level = level * jnp.repeat(jnp.exp(heights), extent[axis_at] // parts).reshape((-1,) + (1,) * (len(extent) - 1 - axis_at))
    return level


def scatter_about(rng, shape, spread, bound, pieces=(), held_as=jnp.bfloat16):
    array = jax.random.normal(rng, shape, jnp.float32) * spread
    if len(pieces) > 0:
        array = block_levels(rng, shape, pieces, -0.22, 0.18) * array
    return jnp.clip(array, min=-bound, max=bound).astype(held_as)


def setup_inputs(seed: int = 0) -> dict:
    arg_keys = jax.random.split(jax.random.key(seed), 15)
    return {
        "tokens": scatter_about(arg_keys[0], (ROWS_ALL, MODEL_WIDTH), 1.0, 6.0, ((0, 64),)),
        "recurrence_branch_weight": scatter_about(arg_keys[1], (MODEL_WIDTH, RECURRENT_WIDTH), MODEL_WIDTH ** -0.5, 0.125, ((0, 32), (1, 8))),
        "gate_branch_weight": scatter_about(arg_keys[2], (MODEL_WIDTH, RECURRENT_WIDTH), MODEL_WIDTH ** -0.5, 0.125, ((0, 32), (1, 8))),
        "convolution_kernel": scatter_about(arg_keys[3], (CONV, RECURRENT_WIDTH), 0.5, 3.0, ((1, 8),)),
        "recurrence_gate_blockwise": scatter_about(arg_keys[4], (LRU_BLOCKS, BLOCK, BLOCK), BLOCK ** -0.5, 0.375, ((0, 8),)),
        "input_gate_blockwise": scatter_about(arg_keys[5], (LRU_BLOCKS, BLOCK, BLOCK), BLOCK ** -0.5, 0.375, ((0, 8),)),
        "channel_decay_param": draw_channel_decay_param(jax.random.fold_in(arg_keys[14], 71), 0),
        "token_decay_shift": draw_token_decay_shift(jax.random.fold_in(arg_keys[14], 71), 0),
        "recurrence_output_weight": scatter_about(arg_keys[8], (RECURRENT_WIDTH, MODEL_WIDTH), (RECURRENT_WIDTH // 16) ** -0.5, 0.5, ((0, 8), (1, 32))),
        "first_norm_gain": jnp.clip(1.0 + 0.18 * jax.random.normal(arg_keys[9], (MODEL_WIDTH,), jnp.float32), 0.1, 1.9),
        "feedforward_gate_weight": scatter_about(arg_keys[10], (MODEL_WIDTH, FF), MODEL_WIDTH ** -0.5, 0.125, ((0, 32), (1, 8))),
        "feedforward_up_weight": scatter_about(arg_keys[11], (MODEL_WIDTH, FF), MODEL_WIDTH ** -0.5, 0.125, ((0, 32), (1, 8))),
        "feedforward_down_weight": scatter_about(arg_keys[12], (FF, MODEL_WIDTH), (FF // 4) ** -0.5, 0.15625, ((0, 8), (1, 32))),
        "second_norm_gain": jnp.clip(1.0 + 0.18 * jax.random.normal(arg_keys[13], (MODEL_WIDTH,), jnp.float32), 0.1, 1.9),
    }


residual_scale = 1.4142135623730951

def layer_norm(values, gain):
    center = values - lax.optimization_barrier(jnp.mean(values, axis=-1, keepdims=True))
    variance = lax.optimization_barrier(jnp.mean(center * center, axis=-1, keepdims=True))
    return center * lax.rsqrt(variance + 1e-05) * gain

def grouped_product(left, right):
    width = left.shape[1] // N_TP
    total = jnp.zeros((left.shape[0], right.shape[1]), jnp.float32)
    for group in range(N_TP):
        term = jnp.dot(left[:, group * width:(group + 1) * width], right[group * width:(group + 1) * width], preferred_element_type=jnp.float32)
        term = lax.optimization_barrier(term.astype(jnp.bfloat16))
        total = total + term.astype(jnp.float32)
    return total

def combine(earlier, later):
    return (earlier[0] * later[0], later[0] * earlier[1] + later[1])

def single_sequence_layer(tokens, decay_added, recurrence_branch_weight, gate_branch_weight, convolution_kernel, recurrence_gate_blockwise, input_gate_blockwise, channel_decay_param, recurrence_output_weight, first_norm_gain, feedforward_gate_weight, feedforward_up_weight, feedforward_down_weight, second_norm_gain):
    length = tokens.shape[0]
    value_in = jnp.dot(tokens, recurrence_branch_weight, preferred_element_type=jnp.float32).astype(jnp.bfloat16)
    gate_in = jnp.dot(tokens, gate_branch_weight, preferred_element_type=jnp.float32).astype(jnp.bfloat16)
    padded = jnp.concatenate([jnp.zeros((CONV - 1, RECURRENT_WIDTH), jnp.float32), value_in.astype(jnp.float32)], axis=0)
    conv = jnp.zeros((length, RECURRENT_WIDTH), jnp.float32)
    for tap in range(CONV):
        conv = conv + padded[tap:tap + length] * convolution_kernel[tap].astype(jnp.float32)
    conv = conv.astype(jnp.bfloat16)
    blocked = conv.astype(jnp.float32).reshape(length, LRU_BLOCKS, BLOCK)
    recurrence_gate_value = jax.nn.sigmoid(jnp.einsum('rnk,nkj->rnj', blocked, recurrence_gate_blockwise.astype(jnp.float32)).reshape(length, RECURRENT_WIDTH))
    inlet = jax.nn.sigmoid(jnp.einsum('rnk,nkj->rnj', blocked, input_gate_blockwise.astype(jnp.float32)).reshape(length, RECURRENT_WIDTH))
    log_decay_factor = -8.0 * recurrence_gate_value * jax.nn.softplus(-channel_decay_param) + decay_added
    decay = jnp.exp(log_decay_factor)
    drive = jnp.sqrt(-jnp.expm1(2.0 * log_decay_factor)) * inlet * conv.astype(jnp.float32)
    _, state = lax.associative_scan(combine, (decay, drive), axis=0)
    branch = (state * jax.nn.gelu(gate_in.astype(jnp.float32))).astype(jnp.bfloat16)
    mix = grouped_product(branch, recurrence_output_weight)
    normed = layer_norm(residual_scale * tokens.astype(jnp.float32) + mix, first_norm_gain).astype(jnp.bfloat16)
    gate = jnp.dot(normed, feedforward_gate_weight, preferred_element_type=jnp.float32)
    upward = jnp.dot(normed, feedforward_up_weight, preferred_element_type=jnp.float32)
    hidden = (jax.nn.silu(gate) * upward).astype(jnp.bfloat16)
    ffn = grouped_product(hidden, feedforward_down_weight)
    return layer_norm(residual_scale * normed.astype(jnp.float32) + ffn, second_norm_gain).astype(jnp.bfloat16)

def reference(tokens, recurrence_branch_weight, gate_branch_weight, convolution_kernel, recurrence_gate_blockwise, input_gate_blockwise, channel_decay_param, token_decay_shift, recurrence_output_weight, first_norm_gain, feedforward_gate_weight, feedforward_up_weight, feedforward_down_weight, second_norm_gain):
    token_count = tokens.shape[0] // SEQUENCE_TOKENS

    def apply_layer(pair):
        return single_sequence_layer(pair[0], pair[1], recurrence_branch_weight, gate_branch_weight, convolution_kernel, recurrence_gate_blockwise, input_gate_blockwise, channel_decay_param, recurrence_output_weight, first_norm_gain, feedforward_gate_weight, feedforward_up_weight, feedforward_down_weight, second_norm_gain)
    layer_result = lax.map(apply_layer, (tokens.reshape(token_count, SEQUENCE_TOKENS, MODEL_WIDTH), token_decay_shift.reshape(token_count, SEQUENCE_TOKENS, RECURRENT_WIDTH)))
    return layer_result.reshape(token_count * SEQUENCE_TOKENS, MODEL_WIDTH)
```

```python
import jax
import jax.numpy as jnp
from jax import lax
from jax.experimental import pallas as pl
from jax.experimental.pallas import tpu as pltpu
from jax.sharding import Mesh
from jax.sharding import PartitionSpec as P

residual_scale = 1.4142135623730951
f32 = jnp.float32
bf16 = jnp.bfloat16
AROUND = ("r", "zh", "zl")
ANY = pl.BlockSpec(memory_space=pl.ANY)
VMEM = pl.BlockSpec(memory_space=pltpu.VMEM)
SMEM = pl.BlockSpec(memory_space=pltpu.SMEM)


def copy_for_each(value, axis):
    copies = jnp.broadcast_to(value, (lax.axis_size(axis), *value.shape))
    return lax.all_to_all(copies, axis, split_axis=0, concat_axis=0, tiled=True)


def mix_kernel(
    place_ref, tokens_ref, weight_hbm, taps_ref, rec_ref, inp_ref, decay_ref, shift_ref,
    branch_ref, weight_ref, a_ref, b_ref, sems,
):
    zh = place_ref[0]
    copies = []
    for rel in range(2):
        for y in range(4):
            copies.append(
                pltpu.make_async_copy(
                    weight_hbm.at[y, :, rel],
                    weight_ref.at[lax.rem(zh + rel, 2), :, y],
                    sems.at[rel * 4 + y],
                )
            )
    for copy in copies:
        copy.start()
    for copy in copies:
        copy.wait()
    length, width = shift_ref.shape
    weight = weight_ref[...].reshape(-1, 2 * width)
    acc = jnp.dot(tokens_ref[...], weight, preferred_element_type=f32).astype(bf16).astype(f32)
    value = acc[:, :width]
    taps = taps_ref[...].astype(f32)
    count = taps.shape[0]
    row = lax.broadcasted_iota(jnp.int32, (length, width), 0)
    conv = value * taps[count - 1 : count, :]
    for back in range(1, count):
        moved = jnp.where(row >= back, pltpu.roll(value, back, 0), 0.0)
        conv = conv + moved * taps[count - 1 - back : count - back, :]
    conv = conv.astype(bf16)
    rate = jax.nn.sigmoid(jnp.dot(conv, rec_ref[...], preferred_element_type=f32))
    inlet = jax.nn.sigmoid(jnp.dot(conv, inp_ref[...], preferred_element_type=f32))
    param = decay_ref[...]
    softplus = jnp.maximum(-param, 0.0) + jnp.log1p(jnp.exp(-jnp.abs(param)))
    log_a = rate * (-8.0 * softplus) + shift_ref[...]
    a = jnp.exp(log_a)
    drive = jnp.sqrt(-jnp.tanh(log_a) * (1.0 + a * a)) * inlet * conv.astype(f32)
    tiles = length // 8
    a = a.reshape(tiles, 8, width)
    b = drive.reshape(tiles, 8, width)
    sub = lax.broadcasted_iota(jnp.int32, (tiles, 8, width), 1)
    for step in (1, 2, 4):
        keep = sub >= step
        b = b + a * jnp.where(keep, pltpu.roll(b, step, 1), 0.0)
        a = a * jnp.where(keep, pltpu.roll(a, step, 1), 1.0)
    a_ref[...] = a
    b_ref[...] = b

    def body(tile, last):
        state = b_ref[tile] + a_ref[tile] * last
        b_ref[tile] = state
        return jnp.broadcast_to(state[7:8, :], (8, width))

    lax.fori_loop(0, tiles, body, jnp.zeros((8, width), f32), unroll=8)
    state = b_ref[...].reshape(length, width)
    branch_ref[...] = (state * jax.nn.gelu(acc[:, width:])).astype(bf16)


def mix(place, tokens, weight, taps, rec, inp, decay, shift):
    length, width = shift.shape
    return pl.pallas_call(
        mix_kernel,
        out_shape=jax.ShapeDtypeStruct((length, width), bf16),
        in_specs=[SMEM, VMEM, ANY, VMEM, VMEM, VMEM, VMEM, VMEM],
        out_specs=VMEM,
        scratch_shapes=[
            pltpu.VMEM((2, 4, 4, tokens.shape[1] // 32, 2 * width), bf16),
            pltpu.VMEM((length // 8, 8, width), f32),
            pltpu.VMEM((length // 8, 8, width), f32),
            pltpu.SemaphoreType.DMA((8,)),
        ],
        name="mix",
        compiler_params=pltpu.CompilerParams(vmem_limit_bytes=40 << 20),
    )(place, tokens, weight, taps, rec, inp, decay.reshape(1, width), shift)


def last_dims(left, right):
    return lax.dot_general(left, right, (((1,), (1,)), ((), ())), preferred_element_type=f32)


def project_kernel(place_ref, branch_ref, weight_hbm, keep_ref, send_ref, weight_ref, sems):
    zh, c = place_ref[0], place_ref[1]
    copies = []
    for rel in range(2):
        for y in range(4):
            copies.append(
                pltpu.make_async_copy(
                    weight_hbm.at[y, :, rel],
                    weight_ref.at[lax.rem(zh + rel, 2), :, y],
                    sems.at[rel * 4 + y],
                )
            )
    for copy in copies:
        copy.start()
    for copy in copies:
        copy.wait()
    share = keep_ref.shape[1]
    weight = weight_ref[...].reshape(-1, branch_ref.shape[1])
    for out_ref, core in ((send_ref, 1 - c), (keep_ref, c)):
        rows = [
            branch_ref[pl.ds(pl.multiple_of((2 * x + core) * share, share), share), :]
            for x in range(keep_ref.shape[0])
        ]
        out = last_dims(jnp.concatenate(rows, axis=0), weight)
        out_ref[...] = out.astype(bf16).reshape(out_ref.shape)


def project(place, branch, weight, share):
    width = branch.shape[1]
    features = weight.size // width
    half = jax.ShapeDtypeStruct((branch.shape[0] // (2 * share), share, features), bf16)
    return pl.pallas_call(
        project_kernel,
        out_shape=(half, half),
        in_specs=[SMEM, VMEM, ANY],
        out_specs=(VMEM, VMEM),
        scratch_shapes=[
            pltpu.VMEM((2, 4, 4, features // 32, width), bf16),
            pltpu.SemaphoreType.DMA((8,)),
        ],
        name="project",
        compiler_params=pltpu.CompilerParams(vmem_limit_bytes=40 << 20),
    )(place, branch, weight)


def norm_kernel(parts_ref, residual_ref, gain_ref, out_ref):
    total = residual_scale * residual_ref[...].astype(f32)
    for x in range(parts_ref.shape[0]):
        total = total + parts_ref[x].astype(f32)
    center = total - jnp.mean(total, axis=-1, keepdims=True)
    variance = jnp.mean(center * center, axis=-1, keepdims=True)
    out_ref[...] = (center * lax.rsqrt(variance + 1e-05) * gain_ref[...]).astype(bf16)


def norm(parts, residual, gain):
    return pl.pallas_call(
        norm_kernel,
        out_shape=jax.ShapeDtypeStruct(residual.shape, bf16),
        in_specs=[VMEM, VMEM, VMEM],
        out_specs=VMEM,
        name="norm",
    )(parts, residual, gain.reshape(1, -1))


def feed_kernel(
    mine_ref, other_ref, weight_hbm, keep_ref, send_ref, gate_ref, up_ref, down_ref, sems
):
    height = gate_ref.shape[2]
    copies = [
        pltpu.make_async_copy(weight_hbm.at[0, :, :, :height], gate_ref, sems.at[0]),
        pltpu.make_async_copy(weight_hbm.at[1, :, :, :height], up_ref, sems.at[1]),
        pltpu.make_async_copy(weight_hbm.at[0, :, :, height:], down_ref.at[:, :, 0], sems.at[2]),
        pltpu.make_async_copy(weight_hbm.at[1, :, :, height:], down_ref.at[:, :, 1], sems.at[3]),
    ]
    for copy in copies:
        copy.start()
    units = gate_ref.shape[-1]
    half, share, features = mine_ref.shape
    rows = jnp.concatenate(
        [
            other_ref[...].reshape(half * share, features),
            mine_ref[...].reshape(half * share, features),
        ],
        axis=0,
    )
    copies[0].wait()
    gate = jnp.dot(rows, gate_ref[...].reshape(-1, units), preferred_element_type=f32)
    copies[1].wait()
    up = jnp.dot(rows, up_ref[...].reshape(-1, units), preferred_element_type=f32)
    hidden = (jax.nn.silu(gate) * up).astype(bf16)
    copies[2].wait()
    copies[3].wait()
    down = down_ref[...].reshape(-1, units)
    send_ref[...] = last_dims(hidden[: half * share], down).astype(bf16).reshape(send_ref.shape)
    keep_ref[...] = last_dims(hidden[half * share :], down).astype(bf16).reshape(keep_ref.shape)


def feed(mine, other, weight):
    units = weight.shape[-1]
    height = weight.shape[3] * 2 // 3
    out = jax.ShapeDtypeStruct(mine.shape, bf16)
    return pl.pallas_call(
        feed_kernel,
        out_shape=(out, out),
        in_specs=[VMEM, VMEM, ANY],
        out_specs=(VMEM, VMEM),
        scratch_shapes=[
            pltpu.VMEM((8, 4, height, units), bf16),
            pltpu.VMEM((8, 4, height, units), bf16),
            pltpu.VMEM((8, 4, 2, height // 2, units), bf16),
            pltpu.SemaphoreType.DMA((4,)),
        ],
        name="feed",
        compiler_params=pltpu.CompilerParams(vmem_limit_bytes=50 << 20),
    )(mine, other, weight)


def to_partner(value):
    return lax.ppermute(value, "c", [(0, 1), (1, 0)])


def shifted(value, by):
    return lax.ppermute(value, AROUND, [(i, (i + by) % 16) for i in range(16)])


def sum_at_owner(keep, send):
    both = (keep.astype(f32) + to_partner(send).astype(f32)).astype(bf16)
    return lax.all_to_all(both, "x", 0, 0, tiled=True)


def local(
    tokens,
    recurrence_branch_weight,
    gate_branch_weight,
    convolution_kernel,
    recurrence_gate_blockwise,
    input_gate_blockwise,
    channel_decay_param,
    token_decay_shift,
    recurrence_output_weight,
    first_norm_gain,
    feedforward_gate_weight,
    feedforward_up_weight,
    feedforward_down_weight,
    second_norm_gain,
):
    length = tokens.shape[0]
    share = length // 8
    r, zh = lax.axis_index("r"), lax.axis_index("zh")
    x, c = lax.axis_index("x"), lax.axis_index("c")
    place = jnp.stack([zh, c]).astype(jnp.int32)
    channels = recurrence_branch_weight.shape[1]

    down = feedforward_down_weight.T
    height = down.shape[0]
    fed = jnp.concatenate(
        [
            jnp.where(r == 0, feedforward_gate_weight, feedforward_up_weight),
            jnp.where(r == 0, down[: height // 2], down[height // 2 :]),
        ],
        axis=0,
    )
    fed_column = copy_for_each(fed, "y")
    fed_all = lax.all_gather(fed_column, AROUND, axis=0, tiled=False)
    fed_all = fed_all.reshape(2, 8, 4, *fed.shape)

    first = jnp.concatenate(
        [recurrence_branch_weight, gate_branch_weight, recurrence_output_weight.T], axis=1
    )
    half = height // 2
    across = jnp.concatenate([shifted(first[:half], 4), shifted(first[half:], -4)], axis=0)
    pair = jnp.stack([first, across])
    line = copy_for_each(pair, "zl")
    branch_weight = copy_for_each(line[..., : 2 * channels], "y")
    output_weight = copy_for_each(line[..., 2 * channels :], "y")

    branch = mix(
        place,
        tokens,
        branch_weight,
        convolution_kernel,
        recurrence_gate_blockwise[0],
        input_gate_blockwise[0],
        channel_decay_param,
        token_decay_shift,
    )
    mixed = sum_at_owner(*project(place, branch, output_weight, share))
    own_tokens = lax.dynamic_slice_in_dim(tokens, (2 * x + c) * share, share, 0)
    normed = norm(mixed, own_tokens, first_norm_gain)
    mine = copy_for_each(normed, "x")
    other = to_partner(mine)
    ffn = sum_at_owner(*feed(mine, other, fed_all))
    return norm(ffn, normed, second_norm_gain)


def solution(mesh):
    fine = Mesh(mesh.devices.reshape(2, 2, 4, 4, 4, 2), ("r", "zh", "zl", "y", "x", "c"))
    fs = ("zh", "zl", "y")
    tp = ("x", "c")
    return jax.shard_map(
        local,
        mesh=fine,
        in_specs=(
            P(("r", *fs), None),
            P(fs, tp),
            P(fs, tp),
            P(None, tp),
            P(tp, None, None),
            P(tp, None, None),
            P(tp),
            P(("r", *fs), tp),
            P(tp, fs),
            P(),
            P(fs, tp),
            P(fs, tp),
            P(tp, fs),
            P(),
        ),
        out_specs=P(("r", *fs, *tp), None),
        check_vma=False,
    )
```

```python
import jax
import jax.numpy as jnp
from jax import lax
from jax.experimental import pallas as pl
from jax.experimental.pallas import tpu as pltpu
from jax.sharding import Mesh
from jax.sharding import PartitionSpec as P

residual_scale = 1.4142135623730951
f32 = jnp.float32
bf16 = jnp.bfloat16
AROUND = ("r", "zh", "zl")
ANY = pl.BlockSpec(memory_space=pl.ANY)
HBM = pl.BlockSpec(memory_space=pltpu.HBM)
VMEM = pl.BlockSpec(memory_space=pltpu.VMEM)
SMEM = pl.BlockSpec(memory_space=pltpu.SMEM)


def copy_for_each(value, axis):
    copies = jnp.broadcast_to(value, (lax.axis_size(axis), *value.shape))
    return lax.all_to_all(copies, axis, split_axis=0, concat_axis=0, tiled=True)


def start_all(copies):
    for copy in copies:
        copy.start()


def wait_all(copies):
    for copy in copies:
        copy.wait()


def mix_kernel(
    tokens_hbm, weight_hbm, taps_ref, rec_ref, inp_ref, decay_ref, shift_hbm,
    branch_ref, tokens_ref, weight_ref, shift_ref, a_ref, b_ref, sems,
):
    first = [
        pltpu.make_async_copy(
            weight_hbm.at[y, :, zh], weight_ref.at[zh, :, y], sems.at[4 * zh + y]
        )
        for zh in range(2)
        for y in range(4)
    ]
    first.append(pltpu.make_async_copy(tokens_hbm, tokens_ref, sems.at[8]))
    late = pltpu.make_async_copy(shift_hbm, shift_ref, sems.at[9])
    start_all(first)
    late.start()
    wait_all(first)
    length, width = shift_ref.shape
    weight = weight_ref[...].reshape(-1, 2 * width)
    acc = jnp.dot(tokens_ref[...], weight, preferred_element_type=f32).astype(bf16).astype(f32)
    value = acc[:, :width]
    taps = taps_ref[...].astype(f32)
    count = taps.shape[0]
    row = lax.broadcasted_iota(jnp.int32, (length, width), 0)
    conv = value * taps[count - 1 : count, :]
    for back in range(1, count):
        moved = jnp.where(row >= back, pltpu.roll(value, back, 0), 0.0)
        conv = conv + moved * taps[count - 1 - back : count - back, :]
    conv = conv.astype(bf16)
    rate = jax.nn.sigmoid(jnp.dot(conv, rec_ref[...], preferred_element_type=f32))
    inlet = jax.nn.sigmoid(jnp.dot(conv, inp_ref[...], preferred_element_type=f32))
    param = decay_ref[...]
    softplus = jnp.maximum(-param, 0.0) + jnp.log1p(jnp.exp(-jnp.abs(param)))
    late.wait()
    log_a = rate * (-8.0 * softplus) + shift_ref[...]
    a = jnp.exp(log_a)
    drive = jnp.sqrt(-jnp.tanh(log_a) * (1.0 + a * a)) * inlet * conv.astype(f32)
    tiles = length // 8
    a = a.reshape(tiles, 8, width)
    b = drive.reshape(tiles, 8, width)
    sub = lax.broadcasted_iota(jnp.int32, (tiles, 8, width), 1)
    for step in (1, 2, 4):
        keep = sub >= step
        b = b + a * jnp.where(keep, pltpu.roll(b, step, 1), 0.0)
        a = a * jnp.where(keep, pltpu.roll(a, step, 1), 1.0)
    a_ref[...] = a
    b_ref[...] = b

    def body(tile, last):
        state = b_ref[tile] + a_ref[tile] * last
        b_ref[tile] = state
        return jnp.broadcast_to(state[7:8, :], (8, width))

    lax.fori_loop(0, tiles, body, jnp.zeros((8, width), f32), unroll=8)
    state = b_ref[...].reshape(length, width)
    branch_ref[...] = (state * jax.nn.gelu(acc[:, width:])).astype(bf16)


def mix(tokens, weight, taps, rec, inp, decay, shift):
    length, width = shift.shape
    return pl.pallas_call(
        mix_kernel,
        out_shape=jax.ShapeDtypeStruct((length, width), bf16),
        in_specs=[HBM, ANY, VMEM, VMEM, VMEM, VMEM, HBM],
        out_specs=VMEM,
        scratch_shapes=[
            pltpu.VMEM(tokens.shape, bf16),
            pltpu.VMEM((2, 4, 4, tokens.shape[1] // 32, 2 * width), bf16),
            pltpu.VMEM(shift.shape, f32),
            pltpu.VMEM((length // 8, 8, width), f32),
            pltpu.VMEM((length // 8, 8, width), f32),
            pltpu.SemaphoreType.DMA((10,)),
        ],
        name="mix",
        compiler_params=pltpu.CompilerParams(vmem_limit_bytes=16 << 20),
    )(tokens, weight, taps, rec, inp, decay.reshape(1, width), shift)


def last_dims(left, right):
    return lax.dot_general(left, right, (((1,), (1,)), ((), ())), preferred_element_type=f32)


def project_kernel(place_ref, branch_ref, weight_hbm, keep_ref, send_ref, weight_ref, sems):
    c = place_ref[0]
    copies = [
        pltpu.make_async_copy(
            weight_hbm.at[y, :, zh], weight_ref.at[zh, :, y], sems.at[4 * zh + y]
        )
        for zh in range(2)
        for y in range(4)
    ]
    start_all(copies)
    wait_all(copies)
    share = keep_ref.shape[1]
    weight = weight_ref[...].reshape(-1, branch_ref.shape[1])
    for out_ref, core in ((send_ref, 1 - c), (keep_ref, c)):
        rows = [
            branch_ref[pl.ds(pl.multiple_of((2 * x + core) * share, share), share), :]
            for x in range(keep_ref.shape[0])
        ]
        out = last_dims(jnp.concatenate(rows, axis=0), weight)
        out_ref[...] = out.astype(bf16).reshape(out_ref.shape)


def project(place, branch, weight, share):
    width = branch.shape[1]
    features = weight.size // width
    half = jax.ShapeDtypeStruct((branch.shape[0] // (2 * share), share, features), bf16)
    return pl.pallas_call(
        project_kernel,
        out_shape=(half, half),
        in_specs=[SMEM, VMEM, ANY],
        out_specs=(VMEM, VMEM),
        scratch_shapes=[
            pltpu.VMEM((2, 4, 4, features // 32, width), bf16),
            pltpu.SemaphoreType.DMA((8,)),
        ],
        name="project",
        compiler_params=pltpu.CompilerParams(vmem_limit_bytes=16 << 20),
    )(place, branch, weight)


def norm_rows(parts_hbm, residual_ref, gain_ref, parts_ref, sem):
    copy = pltpu.make_async_copy(parts_hbm, parts_ref, sem.at[0])
    copy.start()
    total = residual_scale * residual_ref[...].astype(f32)
    copy.wait()
    for x in range(parts_ref.shape[0]):
        total = total + parts_ref[x].astype(f32)
    center = total - jnp.mean(total, axis=-1, keepdims=True)
    variance = jnp.mean(center * center, axis=-1, keepdims=True)
    return (center * lax.rsqrt(variance + 1e-05) * gain_ref[...]).astype(bf16)


def norm_kernel(parts_hbm, residual_ref, gain_ref, out_ref, parts_ref, sem):
    out_ref[...] = norm_rows(parts_hbm, residual_ref, gain_ref, parts_ref, sem)


def copies_kernel(parts_hbm, residual_ref, gain_ref, out_ref, copies_ref, parts_ref, sem):
    out = norm_rows(parts_hbm, residual_ref, gain_ref, parts_ref, sem)
    out_ref[...] = out
    for x in range(copies_ref.shape[0]):
        copies_ref[x] = out


def norm(parts, residual, gain, copied):
    own = jax.ShapeDtypeStruct(residual.shape, bf16)
    copies = jax.ShapeDtypeStruct(parts.shape, bf16)
    return pl.pallas_call(
        copies_kernel if copied else norm_kernel,
        out_shape=(own, copies) if copied else own,
        in_specs=[ANY, VMEM, VMEM],
        out_specs=(VMEM, VMEM) if copied else VMEM,
        scratch_shapes=[pltpu.VMEM(parts.shape, bf16), pltpu.SemaphoreType.DMA((1,))],
        name="norm",
        compiler_params=pltpu.CompilerParams(vmem_limit_bytes=12 << 20),
    )(parts, residual, gain.reshape(1, -1))


def stage_kernel(place_ref, fed_hbm, gate_ref, up_ref, down_ref, sems):
    y = place_ref[1]
    height = gate_ref.shape[2]
    copies = []
    for at, away in enumerate((0, 3, 1, 2)):
        there = lax.rem(y + away, 4)
        for source, target in (
            (fed_hbm.at[0, :, at, :height], gate_ref.at[:, there]),
            (fed_hbm.at[1, :, at, :height], up_ref.at[:, there]),
            (fed_hbm.at[0, :, at, height:], down_ref.at[:, there, 0]),
            (fed_hbm.at[1, :, at, height:], down_ref.at[:, there, 1]),
        ):
            copies.append(pltpu.make_async_copy(source, target, sems.at[len(copies)]))
    start_all(copies)
    wait_all(copies)


def stage(place, fed):
    units = fed.shape[-1]
    height = fed.shape[3] * 2 // 3
    wide = jax.ShapeDtypeStruct((8, 4, height, units), bf16)
    down = jax.ShapeDtypeStruct((8, 4, 2, height // 2, units), bf16)
    return pl.pallas_call(
        stage_kernel,
        out_shape=(wide, wide, down),
        in_specs=[SMEM, HBM],
        out_specs=(VMEM, VMEM, VMEM),
        scratch_shapes=[pltpu.SemaphoreType.DMA((16,))],
        name="stage",
        compiler_params=pltpu.CompilerParams(vmem_limit_bytes=20 << 20),
    )(place, fed)


def feed_kernel(rows_hbm, gate_ref, up_ref, down_ref, out_ref, rows_ref, sem):
    copy = pltpu.make_async_copy(rows_hbm, rows_ref, sem.at[0])
    copy.start()
    copy.wait()
    units = gate_ref.shape[-1]
    rows = rows_ref[...].reshape(-1, rows_ref.shape[-1])
    gate = jnp.dot(rows, gate_ref[...].reshape(-1, units), preferred_element_type=f32)
    up = jnp.dot(rows, up_ref[...].reshape(-1, units), preferred_element_type=f32)
    hidden = (jax.nn.silu(gate) * up).astype(bf16)
    out = last_dims(hidden, down_ref[...].reshape(-1, units))
    out_ref[...] = out.astype(bf16).reshape(out_ref.shape)


def feed(rows, gate, up, down):
    return pl.pallas_call(
        feed_kernel,
        out_shape=jax.ShapeDtypeStruct(rows.shape, bf16),
        in_specs=[ANY, VMEM, VMEM, VMEM],
        out_specs=VMEM,
        scratch_shapes=[pltpu.VMEM(rows.shape, bf16), pltpu.SemaphoreType.DMA((1,))],
        name="feed",
        compiler_params=pltpu.CompilerParams(vmem_limit_bytes=16 << 20),
    )(rows, gate, up, down)


def to_partner(value):
    return lax.ppermute(value, "c", [(0, 1), (1, 0)])


def sideways(value, by):
    return lax.ppermute(value, "y", [(i, (i + by) % 4) for i in range(4)])


def sum_at_owner(keep, send):
    both = (keep.astype(f32) + to_partner(send).astype(f32)).astype(bf16)
    return lax.all_to_all(both, "x", 0, 0, tiled=True)


def local(
    tokens,
    recurrence_branch_weight,
    gate_branch_weight,
    convolution_kernel,
    recurrence_gate_blockwise,
    input_gate_blockwise,
    channel_decay_param,
    token_decay_shift,
    recurrence_output_weight,
    first_norm_gain,
    feedforward_gate_weight,
    feedforward_up_weight,
    feedforward_down_weight,
    second_norm_gain,
):
    length = tokens.shape[0]
    share = length // 8
    r = lax.axis_index("r")
    x, c = lax.axis_index("x"), lax.axis_index("c")
    place = jnp.stack([c, lax.axis_index("y")]).astype(jnp.int32)
    channels = recurrence_branch_weight.shape[1]

    down = feedforward_down_weight.T
    height = down.shape[0]
    fed = jnp.concatenate(
        [
            jnp.where(r == 0, feedforward_gate_weight, feedforward_up_weight),
            jnp.where(r == 0, down[: height // 2], down[height // 2 :]),
        ],
        axis=0,
    )
    moved = [sideways(fed, by) for by in (1, -1, 2)]
    fed_column = jnp.stack([fed, *moved])
    fed_all = lax.all_gather(fed_column, AROUND, axis=0, tiled=False)
    fed_all = fed_all.reshape(2, 8, 4, *fed.shape)

    first = jnp.concatenate(
        [recurrence_branch_weight, gate_branch_weight, recurrence_output_weight.T], axis=1
    )
    pair = copy_for_each(first, "zh")
    line = copy_for_each(pair, "zl")
    branch_weight = copy_for_each(line[..., : 2 * channels], "y")
    output_weight = copy_for_each(line[..., 2 * channels :], "y")

    branch = mix(
        tokens,
        branch_weight,
        convolution_kernel,
        recurrence_gate_blockwise[0],
        input_gate_blockwise[0],
        channel_decay_param,
        token_decay_shift,
    )
    mixed = sum_at_owner(*project(place, branch, output_weight, share))
    own_tokens = lax.dynamic_slice_in_dim(tokens, (2 * x + c) * share, share, 0)
    normed, copies = norm(mixed, own_tokens, first_norm_gain, True)
    mine = lax.all_to_all(copies, "x", 0, 0, tiled=True)
    other = to_partner(mine)
    staged = stage(place, fed_all)
    keep = feed(mine, *staged)
    ffn = sum_at_owner(keep, feed(other, *staged))
    return norm(ffn, normed, second_norm_gain, False)


def solution(mesh):
    fine = Mesh(mesh.devices.reshape(2, 2, 4, 4, 4, 2), ("r", "zh", "zl", "y", "x", "c"))
    fs = ("zh", "zl", "y")
    tp = ("x", "c")
    return jax.shard_map(
        local,
        mesh=fine,
        in_specs=(
            P(("r", *fs), None),
            P(fs, tp),
            P(fs, tp),
            P(None, tp),
            P(tp, None, None),
            P(tp, None, None),
            P(tp),
            P(("r", *fs), tp),
            P(tp, fs),
            P(),
            P(fs, tp),
            P(fs, tp),
            P(tp, fs),
            P(),
        ),
        out_specs=P(("r", *fs, *tp), None),
        check_vma=False,
    )
```

```python
import jax
import jax.numpy as jnp
from jax import lax
from jax.experimental import pallas as pl
from jax.experimental.pallas import tpu as pltpu
from jax.sharding import Mesh
from jax.sharding import PartitionSpec as P

residual_scale = 1.4142135623730951
f32 = jnp.float32
bf16 = jnp.bfloat16
AROUND = ("r", "zh", "zl")
ANY = pl.BlockSpec(memory_space=pl.ANY)
HBM = pl.BlockSpec(memory_space=pltpu.HBM)
VMEM = pl.BlockSpec(memory_space=pltpu.VMEM)
SMEM = pl.BlockSpec(memory_space=pltpu.SMEM)


def copy_for_each(value, axis):
    copies = jnp.broadcast_to(value, (lax.axis_size(axis), *value.shape))
    return lax.all_to_all(copies, axis, split_axis=0, concat_axis=0, tiled=True)


def start_all(copies):
    for copy in copies:
        copy.start()


def wait_all(copies):
    for copy in copies:
        copy.wait()


def loads(pieces, target, y, sems):
    copies = []
    half = target.shape[1] // 2
    for away, piece, begin in zip((0, 3, 1, 2, 2), pieces, (0, 0, 0, 0, half)):
        for zh in range(2):
            rows = pl.ds(begin, piece.shape[0])
            copies.append(
                pltpu.make_async_copy(
                    piece.at[:, zh],
                    target.at[zh, rows, lax.rem(y + away, 4)],
                    sems.at[len(copies)],
                )
            )
    return copies


def mix_kernel(place_ref, tokens_hbm, *refs):
    pieces, refs = refs[:5], refs[5:]
    taps_ref, rec_ref, inp_ref, decay_ref, shift_hbm, branch_ref = refs[:6]
    tokens_ref, weight_ref, shift_ref, a_ref, b_ref, sems = refs[6:]
    first = loads(pieces, weight_ref, place_ref[1], sems)
    first.append(pltpu.make_async_copy(tokens_hbm, tokens_ref, sems.at[10]))
    late = pltpu.make_async_copy(shift_hbm, shift_ref, sems.at[11])
    start_all(first)
    late.start()
    wait_all(first)
    length, width = shift_ref.shape
    weight = weight_ref[...].reshape(-1, 2 * width)
    acc = jnp.dot(tokens_ref[...], weight, preferred_element_type=f32).astype(bf16).astype(f32)
    value = acc[:, :width]
    taps = taps_ref[...].astype(f32)
    count = taps.shape[0]
    row = lax.broadcasted_iota(jnp.int32, (length, width), 0)
    conv = value * taps[count - 1 : count, :]
    for back in range(1, count):
        moved = jnp.where(row >= back, pltpu.roll(value, back, 0), 0.0)
        conv = conv + moved * taps[count - 1 - back : count - back, :]
    conv = conv.astype(bf16)
    rate = jax.nn.sigmoid(jnp.dot(conv, rec_ref[...], preferred_element_type=f32))
    inlet = jax.nn.sigmoid(jnp.dot(conv, inp_ref[...], preferred_element_type=f32))
    param = decay_ref[...]
    softplus = jnp.maximum(-param, 0.0) + jnp.log1p(jnp.exp(-jnp.abs(param)))
    late.wait()
    log_a = rate * (-8.0 * softplus) + shift_ref[...]
    a = jnp.exp(log_a)
    drive = jnp.sqrt(-jnp.tanh(log_a) * (1.0 + a * a)) * inlet * conv.astype(f32)
    tiles = length // 8
    a = a.reshape(tiles, 8, width)
    b = drive.reshape(tiles, 8, width)
    sub = lax.broadcasted_iota(jnp.int32, (tiles, 8, width), 1)
    for step in (1, 2, 4):
        keep = sub >= step
        b = b + a * jnp.where(keep, pltpu.roll(b, step, 1), 0.0)
        a = a * jnp.where(keep, pltpu.roll(a, step, 1), 1.0)
    a_ref[...] = a
    b_ref[...] = b

    def body(tile, last):
        state = b_ref[tile] + a_ref[tile] * last
        b_ref[tile] = state
        return jnp.broadcast_to(state[7:8, :], (8, width))

    lax.fori_loop(0, tiles, body, jnp.zeros((8, width), f32), unroll=8)
    state = b_ref[...].reshape(length, width)
    branch_ref[...] = (state * jax.nn.gelu(acc[:, width:])).astype(bf16)


def mix(place, tokens, pieces, taps, rec, inp, decay, shift):
    length, width = shift.shape
    return pl.pallas_call(
        mix_kernel,
        out_shape=jax.ShapeDtypeStruct((length, width), bf16),
        in_specs=[SMEM, HBM] + [ANY] * 5 + [VMEM] * 4 + [HBM],
        out_specs=VMEM,
        scratch_shapes=[
            pltpu.VMEM(tokens.shape, bf16),
            pltpu.VMEM((2, 4, 4, tokens.shape[1] // 32, 2 * width), bf16),
            pltpu.VMEM(shift.shape, f32),
            pltpu.VMEM((length // 8, 8, width), f32),
            pltpu.VMEM((length // 8, 8, width), f32),
            pltpu.SemaphoreType.DMA((12,)),
        ],
        name="mix",
        compiler_params=pltpu.CompilerParams(vmem_limit_bytes=60 << 20),
    )(place, tokens, *pieces, taps, rec, inp, decay.reshape(1, width), shift)


def last_dims(left, right):
    return lax.dot_general(left, right, (((1,), (1,)), ((), ())), preferred_element_type=f32)


def project_kernel(place_ref, branch_ref, *refs):
    pieces, (out_ref, weight_ref, sems) = refs[:5], refs[5:]
    core = place_ref[0]
    copies = loads(pieces, weight_ref, place_ref[1], sems)
    start_all(copies)
    share = out_ref.shape[1]
    rows = [
        branch_ref[pl.ds(pl.multiple_of((2 * x + core) * share, share), share), :]
        for x in range(out_ref.shape[0])
    ]
    wait_all(copies)
    out = last_dims(
        jnp.concatenate(rows, axis=0), weight_ref[...].reshape(-1, branch_ref.shape[1])
    )
    out_ref[...] = out.astype(bf16).reshape(out_ref.shape)


def project(place, branch, pieces, share):
    width = branch.shape[1]
    features = 4 * pieces[0].size // width
    return pl.pallas_call(
        project_kernel,
        out_shape=jax.ShapeDtypeStruct((branch.shape[0] // (2 * share), share, features), bf16),
        in_specs=[SMEM, VMEM] + [ANY] * 5,
        out_specs=VMEM,
        scratch_shapes=[
            pltpu.VMEM((2, 4, 4, features // 32, width), bf16),
            pltpu.SemaphoreType.DMA((10,)),
        ],
        name="project",
        compiler_params=pltpu.CompilerParams(vmem_limit_bytes=16 << 20),
    )(place, branch, *pieces)


def norm_rows(parts_hbm, residual_ref, gain_ref, parts_ref, sem):
    copy = pltpu.make_async_copy(parts_hbm, parts_ref, sem.at[0])
    copy.start()
    total = residual_scale * residual_ref[...].astype(f32)
    copy.wait()
    for x in range(parts_ref.shape[0]):
        total = total + parts_ref[x].astype(f32)
    center = total - jnp.mean(total, axis=-1, keepdims=True)
    variance = jnp.mean(center * center, axis=-1, keepdims=True)
    return (center * lax.rsqrt(variance + 1e-05) * gain_ref[...]).astype(bf16)


def norm_kernel(parts_hbm, residual_ref, gain_ref, out_ref, parts_ref, sem):
    out_ref[...] = norm_rows(parts_hbm, residual_ref, gain_ref, parts_ref, sem)


def copies_kernel(parts_hbm, residual_ref, gain_ref, out_ref, copies_ref, parts_ref, sem):
    out = norm_rows(parts_hbm, residual_ref, gain_ref, parts_ref, sem)
    out_ref[...] = out
    for x in range(copies_ref.shape[0]):
        copies_ref[x] = out


def norm(parts, residual, gain, copied):
    own = jax.ShapeDtypeStruct(residual.shape, bf16)
    copies = jax.ShapeDtypeStruct(parts.shape, bf16)
    return pl.pallas_call(
        copies_kernel if copied else norm_kernel,
        out_shape=(own, copies) if copied else own,
        in_specs=[ANY, VMEM, VMEM],
        out_specs=(VMEM, VMEM) if copied else VMEM,
        scratch_shapes=[pltpu.VMEM(parts.shape, bf16), pltpu.SemaphoreType.DMA((1,))],
        name="norm",
        compiler_params=pltpu.CompilerParams(vmem_limit_bytes=12 << 20),
    )(parts, residual, gain.reshape(1, -1))


def stage_kernel(place_ref, fed_hbm, gate_ref, up_ref, down_ref, sems):
    y = place_ref[1]
    height = gate_ref.shape[2]
    copies = []
    for at, away in enumerate((0, 3, 1, 2)):
        there = lax.rem(y + away, 4)
        for source, target in (
            (fed_hbm.at[0, :, at, :height], gate_ref.at[:, there]),
            (fed_hbm.at[1, :, at, :height], up_ref.at[:, there]),
            (fed_hbm.at[0, :, at, height:], down_ref.at[:, there, 0]),
            (fed_hbm.at[1, :, at, height:], down_ref.at[:, there, 1]),
        ):
            copies.append(pltpu.make_async_copy(source, target, sems.at[len(copies)]))
    start_all(copies)
    wait_all(copies)


def stage(place, fed):
    units = fed.shape[-1]
    height = fed.shape[3] * 2 // 3
    wide = jax.ShapeDtypeStruct((8, 4, height, units), bf16)
    down = jax.ShapeDtypeStruct((8, 4, 2, height // 2, units), bf16)
    return pl.pallas_call(
        stage_kernel,
        out_shape=(wide, wide, down),
        in_specs=[SMEM, HBM],
        out_specs=(VMEM, VMEM, VMEM),
        scratch_shapes=[pltpu.SemaphoreType.DMA((16,))],
        name="stage",
        compiler_params=pltpu.CompilerParams(vmem_limit_bytes=46 << 20),
    )(place, fed)


def feed_kernel(rows_hbm, gate_ref, up_ref, down_ref, out_ref, rows_ref, sem):
    copy = pltpu.make_async_copy(rows_hbm, rows_ref, sem.at[0])
    copy.start()
    copy.wait()
    units = gate_ref.shape[-1]
    rows = rows_ref[...].reshape(-1, rows_ref.shape[-1])
    gate = jnp.dot(rows, gate_ref[...].reshape(-1, units), preferred_element_type=f32)
    up = jnp.dot(rows, up_ref[...].reshape(-1, units), preferred_element_type=f32)
    hidden = (jax.nn.silu(gate) * up).astype(bf16)
    out = last_dims(hidden, down_ref[...].reshape(-1, units))
    out_ref[...] = out.astype(bf16).reshape(out_ref.shape)


def feed(rows, gate, up, down):
    return pl.pallas_call(
        feed_kernel,
        out_shape=jax.ShapeDtypeStruct(rows.shape, bf16),
        in_specs=[ANY, VMEM, VMEM, VMEM],
        out_specs=VMEM,
        scratch_shapes=[pltpu.VMEM(rows.shape, bf16), pltpu.SemaphoreType.DMA((1,))],
        name="feed",
        compiler_params=pltpu.CompilerParams(vmem_limit_bytes=16 << 20),
    )(rows, gate, up, down)


def to_partner(value):
    return lax.ppermute(value, "c", [(0, 1), (1, 0)])


def sideways(value, by):
    return lax.ppermute(value, "y", [(i, (i + by) % 4) for i in range(4)])


def round_y(line):
    after, before = sideways(line, 1), sideways(line, -1)
    middle = line.shape[0] // 2
    far = sideways(after[:middle], 1), sideways(before[middle:], -1)
    return (line, after, before, *far)


def sum_at_owner(keep, send):
    both = (keep.astype(f32) + to_partner(send).astype(f32)).astype(bf16)
    return lax.all_to_all(both, "x", 0, 0, tiled=True)


def local(
    tokens,
    recurrence_branch_weight,
    gate_branch_weight,
    convolution_kernel,
    recurrence_gate_blockwise,
    input_gate_blockwise,
    channel_decay_param,
    token_decay_shift,
    recurrence_output_weight,
    first_norm_gain,
    feedforward_gate_weight,
    feedforward_up_weight,
    feedforward_down_weight,
    second_norm_gain,
):
    length = tokens.shape[0]
    share = length // 8
    r = lax.axis_index("r")
    x, c = lax.axis_index("x"), lax.axis_index("c")
    y = lax.axis_index("y")
    place = jnp.stack([c, y]).astype(jnp.int32)
    partner = jnp.stack([1 - c, y]).astype(jnp.int32)
    channels = recurrence_branch_weight.shape[1]

    down = feedforward_down_weight.T
    height = down.shape[0]
    fed = jnp.concatenate(
        [
            jnp.where(r == 0, feedforward_gate_weight, feedforward_up_weight),
            jnp.where(r == 0, down[: height // 2], down[height // 2 :]),
        ],
        axis=0,
    )
    fed = lax.optimization_barrier(fed)
    moved = [sideways(fed, by) for by in (1, -1, 2)]
    fed_column = jnp.stack([fed, *moved])
    fed_all = lax.all_gather(fed_column, AROUND, axis=0, tiled=False)
    fed_all = fed_all.reshape(2, 8, 4, *fed.shape)

    first = jnp.concatenate(
        [recurrence_branch_weight, gate_branch_weight, recurrence_output_weight.T], axis=1
    )
    pair = copy_for_each(first, "zh")
    line = copy_for_each(pair, "zl")
    branch_weight = round_y(line[..., : 2 * channels])
    output_weight = round_y(line[..., 2 * channels :])

    branch = mix(
        place,
        tokens,
        branch_weight,
        convolution_kernel,
        recurrence_gate_blockwise[0],
        input_gate_blockwise[0],
        channel_decay_param,
        token_decay_shift,
    )
    send = project(partner, branch, output_weight, share)
    mixed = sum_at_owner(project(place, branch, output_weight, share), send)
    own_tokens = lax.dynamic_slice_in_dim(tokens, (2 * x + c) * share, share, 0)
    normed, copies = norm(mixed, own_tokens, first_norm_gain, True)
    mine = lax.all_to_all(copies, "x", 0, 0, tiled=True)
    other = to_partner(mine)
    staged = stage(place, fed_all)
    keep = feed(mine, *staged)
    ffn = sum_at_owner(keep, feed(other, *staged))
    return norm(ffn, normed, second_norm_gain, False)


def solution(mesh):
    fine = Mesh(mesh.devices.reshape(2, 2, 4, 4, 4, 2), ("r", "zh", "zl", "y", "x", "c"))
    fs = ("zh", "zl", "y")
    tp = ("x", "c")
    return jax.shard_map(
        local,
        mesh=fine,
        in_specs=(
            P(("r", *fs), None),
            P(fs, tp),
            P(fs, tp),
            P(None, tp),
            P(tp, None, None),
            P(tp, None, None),
            P(tp),
            P(("r", *fs), tp),
            P(tp, fs),
            P(),
            P(fs, tp),
            P(fs, tp),
            P(tp, fs),
            P(),
        ),
        out_specs=P(("r", *fs, *tp), None),
        check_vma=False,
    )
```

```python
import jax
import jax.numpy as jnp
from jax import lax
from jax.experimental import pallas as pl
from jax.experimental.pallas import tpu as pltpu
from jax.sharding import Mesh
from jax.sharding import PartitionSpec as P

residual_scale = 1.4142135623730951
f32 = jnp.float32
bf16 = jnp.bfloat16
AROUND = ("r", "zh", "zl")
ANY = pl.BlockSpec(memory_space=pl.ANY)
HBM = pl.BlockSpec(memory_space=pltpu.HBM)
VMEM = pl.BlockSpec(memory_space=pltpu.VMEM)
SMEM = pl.BlockSpec(memory_space=pltpu.SMEM)


def copy_for_each(value, axis):
    copies = jnp.broadcast_to(value, (lax.axis_size(axis), *value.shape))
    return lax.all_to_all(copies, axis, split_axis=0, concat_axis=0, tiled=True)


def start_all(copies):
    for copy in copies:
        copy.start()


def wait_all(copies):
    for copy in copies:
        copy.wait()


def loads(pieces, target, y, sems):
    copies = []
    half = target.shape[1] // 2
    for away, piece, begin in zip((0, 3, 1, 2, 2), pieces, (0, 0, 0, 0, half)):
        for zh in range(2):
            rows = pl.ds(begin, piece.shape[0])
            copies.append(
                pltpu.make_async_copy(
                    piece.at[:, zh],
                    target.at[zh, rows, lax.rem(y + away, 4)],
                    sems.at[len(copies)],
                )
            )
    return copies


def mix_kernel(place_ref, tokens_hbm, *refs):
    pieces, refs = refs[:5], refs[5:]
    taps_ref, rec_ref, inp_ref, decay_ref, shift_hbm, branch_ref = refs[:6]
    tokens_ref, weight_ref, shift_ref, a_ref, b_ref, sems = refs[6:]
    first = loads(pieces, weight_ref, place_ref[1], sems)
    first.append(pltpu.make_async_copy(tokens_hbm, tokens_ref, sems.at[10]))
    late = pltpu.make_async_copy(shift_hbm, shift_ref, sems.at[11])
    start_all(first)
    late.start()
    wait_all(first)
    length, width = shift_ref.shape
    weight = weight_ref[...].reshape(-1, 2 * width)
    acc = jnp.dot(tokens_ref[...], weight, preferred_element_type=f32).astype(bf16).astype(f32)
    value = acc[:, :width]
    taps = taps_ref[...].astype(f32)
    count = taps.shape[0]
    row = lax.broadcasted_iota(jnp.int32, (length, width), 0)
    conv = value * taps[count - 1 : count, :]
    for back in range(1, count):
        moved = jnp.where(row >= back, pltpu.roll(value, back, 0), 0.0)
        conv = conv + moved * taps[count - 1 - back : count - back, :]
    conv = conv.astype(bf16)
    rate = jax.nn.sigmoid(jnp.dot(conv, rec_ref[...], preferred_element_type=f32))
    inlet = jax.nn.sigmoid(jnp.dot(conv, inp_ref[...], preferred_element_type=f32))
    param = decay_ref[...]
    softplus = jnp.maximum(-param, 0.0) + jnp.log1p(jnp.exp(-jnp.abs(param)))
    late.wait()
    log_a = rate * (-8.0 * softplus) + shift_ref[...]
    a = jnp.exp(log_a)
    drive = jnp.sqrt(-jnp.tanh(log_a) * (1.0 + a * a)) * inlet * conv.astype(f32)
    tiles = length // 8
    a = a.reshape(tiles, 8, width)
    b = drive.reshape(tiles, 8, width)
    sub = lax.broadcasted_iota(jnp.int32, (tiles, 8, width), 1)
    for step in (1, 2, 4):
        keep = sub >= step
        b = b + a * jnp.where(keep, pltpu.roll(b, step, 1), 0.0)
        a = a * jnp.where(keep, pltpu.roll(a, step, 1), 1.0)
    a_ref[...] = a
    b_ref[...] = b

    def body(tile, last):
        state = b_ref[tile] + a_ref[tile] * last
        b_ref[tile] = state
        return jnp.broadcast_to(state[7:8, :], (8, width))

    lax.fori_loop(0, tiles, body, jnp.zeros((8, width), f32), unroll=8)
    state = b_ref[...].reshape(length, width)
    branch_ref[...] = (state * jax.nn.gelu(acc[:, width:])).astype(bf16)


def mix(place, tokens, pieces, taps, rec, inp, decay, shift):
    length, width = shift.shape
    return pl.pallas_call(
        mix_kernel,
        out_shape=jax.ShapeDtypeStruct((length, width), bf16),
        in_specs=[SMEM, HBM] + [ANY] * 5 + [VMEM] * 4 + [HBM],
        out_specs=VMEM,
        scratch_shapes=[
            pltpu.VMEM(tokens.shape, bf16),
            pltpu.VMEM((2, 4, 4, tokens.shape[1] // 32, 2 * width), bf16),
            pltpu.VMEM(shift.shape, f32),
            pltpu.VMEM((length // 8, 8, width), f32),
            pltpu.VMEM((length // 8, 8, width), f32),
            pltpu.SemaphoreType.DMA((12,)),
        ],
        name="mix",
        compiler_params=pltpu.CompilerParams(vmem_limit_bytes=16 << 20),
    )(place, tokens, *pieces, taps, rec, inp, decay.reshape(1, width), shift)


def last_dims(left, right):
    return lax.dot_general(left, right, (((1,), (1,)), ((), ())), preferred_element_type=f32)


def project_kernel(place_ref, branch_hbm, *refs):
    pieces, (out_ref, branch_ref, weight_ref, sems) = refs[:5], refs[5:]
    core = place_ref[0]
    copies = loads(pieces, weight_ref, place_ref[1], sems)
    whole = pltpu.make_async_copy(branch_hbm, branch_ref, sems.at[len(copies)])
    whole.start()
    start_all(copies)
    share = out_ref.shape[1]
    whole.wait()
    rows = [
        branch_ref[pl.ds(pl.multiple_of((2 * x + core) * share, share), share), :]
        for x in range(out_ref.shape[0])
    ]
    wait_all(copies)
    out = last_dims(
        jnp.concatenate(rows, axis=0), weight_ref[...].reshape(-1, branch_ref.shape[1])
    )
    out_ref[...] = out.astype(bf16).reshape(out_ref.shape)


def project(place, branch, pieces, share):
    width = branch.shape[1]
    features = 4 * pieces[0].size // width
    return pl.pallas_call(
        project_kernel,
        out_shape=jax.ShapeDtypeStruct((branch.shape[0] // (2 * share), share, features), bf16),
        in_specs=[SMEM, ANY] + [ANY] * 5,
        out_specs=VMEM,
        scratch_shapes=[
            pltpu.VMEM(branch.shape, bf16),
            pltpu.VMEM((2, 4, 4, features // 32, width), bf16),
            pltpu.SemaphoreType.DMA((11,)),
        ],
        name="project",
        compiler_params=pltpu.CompilerParams(vmem_limit_bytes=16 << 20),
    )(place, branch, *pieces)


def norm_rows(parts_hbm, residual_ref, gain_ref, parts_ref, sem):
    copy = pltpu.make_async_copy(parts_hbm, parts_ref, sem.at[0])
    copy.start()
    total = residual_scale * residual_ref[...].astype(f32)
    copy.wait()
    for x in range(parts_ref.shape[0]):
        total = total + parts_ref[x].astype(f32)
    center = total - jnp.mean(total, axis=-1, keepdims=True)
    variance = jnp.mean(center * center, axis=-1, keepdims=True)
    return (center * lax.rsqrt(variance + 1e-05) * gain_ref[...]).astype(bf16)


def norm_kernel(parts_hbm, residual_ref, gain_ref, out_ref, parts_ref, sem):
    out_ref[...] = norm_rows(parts_hbm, residual_ref, gain_ref, parts_ref, sem)


def copies_kernel(parts_hbm, residual_ref, gain_ref, out_ref, copies_ref, parts_ref, sem):
    out = norm_rows(parts_hbm, residual_ref, gain_ref, parts_ref, sem)
    out_ref[...] = out
    for x in range(copies_ref.shape[0]):
        copies_ref[x] = out


def norm(parts, residual, gain, copied):
    own = jax.ShapeDtypeStruct(residual.shape, bf16)
    copies = jax.ShapeDtypeStruct(parts.shape, bf16)
    return pl.pallas_call(
        copies_kernel if copied else norm_kernel,
        out_shape=(own, copies) if copied else own,
        in_specs=[ANY, VMEM, VMEM],
        out_specs=(VMEM, VMEM) if copied else VMEM,
        scratch_shapes=[pltpu.VMEM(parts.shape, bf16), pltpu.SemaphoreType.DMA((1,))],
        name="norm",
        compiler_params=pltpu.CompilerParams(vmem_limit_bytes=12 << 20),
    )(parts, residual, gain.reshape(1, -1))


def stage_kernel(place_ref, fed_hbm, gate_ref, up_ref, down_ref, sems):
    y = place_ref[1]
    height = gate_ref.shape[2]
    copies = []
    for at, away in enumerate((0, 3, 1, 2)):
        there = lax.rem(y + away, 4)
        for source, target in (
            (fed_hbm.at[0, :, at, :height], gate_ref.at[:, there]),
            (fed_hbm.at[1, :, at, :height], up_ref.at[:, there]),
            (fed_hbm.at[0, :, at, height:], down_ref.at[:, there, 0]),
            (fed_hbm.at[1, :, at, height:], down_ref.at[:, there, 1]),
        ):
            copies.append(pltpu.make_async_copy(source, target, sems.at[len(copies)]))
    start_all(copies)
    wait_all(copies)


def stage(place, fed):
    units = fed.shape[-1]
    height = fed.shape[3] * 2 // 3
    wide = jax.ShapeDtypeStruct((8, 4, height, units), bf16)
    down = jax.ShapeDtypeStruct((8, 4, 2, height // 2, units), bf16)
    return pl.pallas_call(
        stage_kernel,
        out_shape=(wide, wide, down),
        in_specs=[SMEM, HBM],
        out_specs=(VMEM, VMEM, VMEM),
        scratch_shapes=[pltpu.SemaphoreType.DMA((16,))],
        name="stage",
        compiler_params=pltpu.CompilerParams(vmem_limit_bytes=46 << 20),
    )(place, fed)


def feed_kernel(rows_hbm, gate_ref, up_ref, down_ref, out_ref, rows_ref, sem):
    copy = pltpu.make_async_copy(rows_hbm, rows_ref, sem.at[0])
    copy.start()
    copy.wait()
    units = gate_ref.shape[-1]
    rows = rows_ref[...].reshape(-1, rows_ref.shape[-1])
    gate = jnp.dot(rows, gate_ref[...].reshape(-1, units), preferred_element_type=f32)
    up = jnp.dot(rows, up_ref[...].reshape(-1, units), preferred_element_type=f32)
    hidden = (jax.nn.silu(gate) * up).astype(bf16)
    out = last_dims(hidden, down_ref[...].reshape(-1, units))
    out_ref[...] = out.astype(bf16).reshape(out_ref.shape)


def feed(rows, gate, up, down):
    return pl.pallas_call(
        feed_kernel,
        out_shape=jax.ShapeDtypeStruct(rows.shape, bf16),
        in_specs=[ANY, VMEM, VMEM, VMEM],
        out_specs=VMEM,
        scratch_shapes=[pltpu.VMEM(rows.shape, bf16), pltpu.SemaphoreType.DMA((1,))],
        name="feed",
        compiler_params=pltpu.CompilerParams(vmem_limit_bytes=16 << 20),
    )(rows, gate, up, down)


def to_partner(value):
    return lax.ppermute(value, "c", [(0, 1), (1, 0)])


def sideways(value, by):
    return lax.ppermute(value, "y", [(i, (i + by) % 4) for i in range(4)])


def round_y(line):
    after, before = sideways(line, 1), sideways(line, -1)
    middle = line.shape[0] // 2
    far = sideways(after[:middle], 1), sideways(before[middle:], -1)
    return (line, after, before, *far)


def sum_at_owner(keep, send):
    both = (keep.astype(f32) + to_partner(send).astype(f32)).astype(bf16)
    return lax.all_to_all(both, "x", 0, 0, tiled=True)


def local(
    tokens,
    recurrence_branch_weight,
    gate_branch_weight,
    convolution_kernel,
    recurrence_gate_blockwise,
    input_gate_blockwise,
    channel_decay_param,
    token_decay_shift,
    recurrence_output_weight,
    first_norm_gain,
    feedforward_gate_weight,
    feedforward_up_weight,
    feedforward_down_weight,
    second_norm_gain,
):
    length = tokens.shape[0]
    share = length // 8
    r = lax.axis_index("r")
    x, c = lax.axis_index("x"), lax.axis_index("c")
    y = lax.axis_index("y")
    place = jnp.stack([c, y]).astype(jnp.int32)
    partner = jnp.stack([1 - c, y]).astype(jnp.int32)
    channels = recurrence_branch_weight.shape[1]

    own_tokens = lax.dynamic_slice_in_dim(tokens, (2 * x + c) * share, share, 0)

    down = feedforward_down_weight.T
    height = down.shape[0]
    fed = jnp.concatenate(
        [
            jnp.where(r == 0, feedforward_gate_weight, feedforward_up_weight),
            jnp.where(r == 0, down[: height // 2], down[height // 2 :]),
        ],
        axis=0,
    )
    fed = lax.optimization_barrier(fed)
    moved = [sideways(fed, by) for by in (1, -1, 2)]
    fed_column = jnp.stack([fed, *moved])
    fed_all = lax.all_gather(fed_column, AROUND, axis=0, tiled=False)
    fed_all = fed_all.reshape(2, 8, 4, *fed.shape)

    first = jnp.concatenate(
        [recurrence_branch_weight, gate_branch_weight, recurrence_output_weight.T], axis=1
    )
    pair = copy_for_each(first, "zh")
    line = copy_for_each(pair, "zl")
    branch_weight = round_y(line[..., : 2 * channels])
    output_weight = round_y(line[..., 2 * channels :])

    branch = mix(
        place,
        tokens,
        branch_weight,
        convolution_kernel,
        recurrence_gate_blockwise[0],
        input_gate_blockwise[0],
        channel_decay_param,
        token_decay_shift,
    )
    send = project(partner, branch, output_weight, share)
    mixed = sum_at_owner(project(place, branch, output_weight, share), send)
    normed, copies = norm(mixed, own_tokens, first_norm_gain, True)
    mine = lax.all_to_all(copies, "x", 0, 0, tiled=True)
    other = to_partner(mine)
    staged = stage(place, fed_all)
    keep = feed(mine, *staged)
    ffn = sum_at_owner(keep, feed(other, *staged))
    return norm(ffn, normed, second_norm_gain, False)


def solution(mesh):
    fine = Mesh(mesh.devices.reshape(2, 2, 4, 4, 4, 2), ("r", "zh", "zl", "y", "x", "c"))
    fs = ("zh", "zl", "y")
    tp = ("x", "c")
    return jax.shard_map(
        local,
        mesh=fine,
        in_specs=(
            P(("r", *fs), None),
            P(fs, tp),
            P(fs, tp),
            P(None, tp),
            P(tp, None, None),
            P(tp, None, None),
            P(tp),
            P(("r", *fs), tp),
            P(tp, fs),
            P(),
            P(fs, tp),
            P(fs, tp),
            P(tp, fs),
            P(),
        ),
        out_specs=P(("r", *fs, *tp), None),
        check_vma=False,
    )
```

```python
import jax
import jax.numpy as jnp
from jax import lax
from jax.experimental import pallas as pl
from jax.experimental.pallas import tpu as pltpu
from jax.sharding import Mesh
from jax.sharding import PartitionSpec as P

residual_scale = 1.4142135623730951
f32 = jnp.float32
bf16 = jnp.bfloat16
AROUND = ("r", "zh", "zl")
ANY = pl.BlockSpec(memory_space=pl.ANY)
HBM = pl.BlockSpec(memory_space=pltpu.HBM)
VMEM = pl.BlockSpec(memory_space=pltpu.VMEM)
SMEM = pl.BlockSpec(memory_space=pltpu.SMEM)


def copy_for_each(value, axis):
    copies = jnp.broadcast_to(value, (lax.axis_size(axis), *value.shape))
    return lax.all_to_all(copies, axis, split_axis=0, concat_axis=0, tiled=True)


def start_all(copies):
    for copy in copies:
        copy.start()


def wait_all(copies):
    for copy in copies:
        copy.wait()


def loads(pieces, target, y, sems):
    copies = []
    half = target.shape[1] // 2
    for away, piece, begin in zip((0, 3, 1, 2, 2), pieces, (0, 0, 0, 0, half)):
        for zh in range(2):
            rows = pl.ds(begin, piece.shape[0])
            copies.append(
                pltpu.make_async_copy(
                    piece.at[:, zh],
                    target.at[zh, rows, lax.rem(y + away, 4)],
                    sems.at[len(copies)],
                )
            )
    return copies


def mix_kernel(place_ref, tokens_hbm, *refs):
    pieces, refs = refs[:5], refs[5:]
    taps_ref, rec_ref, inp_ref, decay_ref, shift_hbm, branch_ref = refs[:6]
    tokens_ref, weight_ref, shift_ref, a_ref, b_ref, sems = refs[6:]
    first = loads(pieces, weight_ref, place_ref[1], sems)
    first.append(pltpu.make_async_copy(tokens_hbm, tokens_ref, sems.at[10]))
    late = pltpu.make_async_copy(shift_hbm, shift_ref, sems.at[11])
    start_all(first)
    late.start()
    wait_all(first)
    length, width = shift_ref.shape
    weight = weight_ref[...].reshape(-1, 2 * width)
    acc = jnp.dot(tokens_ref[...], weight, preferred_element_type=f32).astype(bf16).astype(f32)
    value = acc[:, :width]
    taps = taps_ref[...].astype(f32)
    count = taps.shape[0]
    row = lax.broadcasted_iota(jnp.int32, (length, width), 0)
    conv = value * taps[count - 1 : count, :]
    for back in range(1, count):
        moved = jnp.where(row >= back, pltpu.roll(value, back, 0), 0.0)
        conv = conv + moved * taps[count - 1 - back : count - back, :]
    conv = conv.astype(bf16)
    rate = jax.nn.sigmoid(jnp.dot(conv, rec_ref[...], preferred_element_type=f32))
    inlet = jax.nn.sigmoid(jnp.dot(conv, inp_ref[...], preferred_element_type=f32))
    param = decay_ref[...]
    softplus = jnp.maximum(-param, 0.0) + jnp.log1p(jnp.exp(-jnp.abs(param)))
    late.wait()
    log_a = -8.0 * rate * softplus + shift_ref[...]
    a = jnp.exp(log_a)
    drive = jnp.sqrt(-jnp.tanh(log_a) * (1.0 + a * a)) * inlet * conv.astype(f32)
    tiles = length // 8
    a = a.reshape(tiles, 8, width)
    b = drive.reshape(tiles, 8, width)
    sub = lax.broadcasted_iota(jnp.int32, (tiles, 8, width), 1)
    for step in (1, 2, 4):
        keep = sub >= step
        b = b + a * jnp.where(keep, pltpu.roll(b, step, 1), 0.0)
        a = a * jnp.where(keep, pltpu.roll(a, step, 1), 1.0)
    a_ref[...] = a
    b_ref[...] = b

    def body(tile, last):
        state = b_ref[tile] + a_ref[tile] * last
        b_ref[tile] = state
        return jnp.broadcast_to(state[7:8, :], (8, width))

    lax.fori_loop(0, tiles, body, jnp.zeros((8, width), f32), unroll=8)
    state = b_ref[...].reshape(length, width)
    branch_ref[...] = (state * jax.nn.gelu(acc[:, width:])).astype(bf16)


def mix(place, tokens, pieces, taps, rec, inp, decay, shift):
    length, width = shift.shape
    return pl.pallas_call(
        mix_kernel,
        out_shape=jax.ShapeDtypeStruct((length, width), bf16),
        in_specs=[SMEM, HBM] + [ANY] * 5 + [VMEM] * 4 + [HBM],
        out_specs=VMEM,
        scratch_shapes=[
            pltpu.VMEM(tokens.shape, bf16),
            pltpu.VMEM((2, 4, 4, tokens.shape[1] // 32, 2 * width), bf16),
            pltpu.VMEM(shift.shape, f32),
            pltpu.VMEM((length // 8, 8, width), f32),
            pltpu.VMEM((length // 8, 8, width), f32),
            pltpu.SemaphoreType.DMA((12,)),
        ],
        name="mix",
        compiler_params=pltpu.CompilerParams(vmem_limit_bytes=16 << 20),
    )(place, tokens, *pieces, taps, rec, inp, decay.reshape(1, width), shift)


def last_dims(left, right):
    return lax.dot_general(left, right, (((1,), (1,)), ((), ())), preferred_element_type=f32)


def project_kernel(place_ref, branch_hbm, *refs):
    pieces, (out_ref, branch_ref, weight_ref, sems) = refs[:5], refs[5:]
    core = place_ref[0]
    copies = loads(pieces, weight_ref, place_ref[1], sems)
    whole = pltpu.make_async_copy(branch_hbm, branch_ref, sems.at[len(copies)])
    whole.start()
    start_all(copies)
    share = out_ref.shape[1]
    whole.wait()
    rows = [
        branch_ref[pl.ds(pl.multiple_of((2 * x + core) * share, share), share), :]
        for x in range(out_ref.shape[0])
    ]
    wait_all(copies)
    out = last_dims(
        jnp.concatenate(rows, axis=0), weight_ref[...].reshape(-1, branch_ref.shape[1])
    )
    out_ref[...] = out.astype(bf16).reshape(out_ref.shape)


def project(place, branch, pieces, share):
    width = branch.shape[1]
    features = 4 * pieces[0].size // width
    return pl.pallas_call(
        project_kernel,
        out_shape=jax.ShapeDtypeStruct((branch.shape[0] // (2 * share), share, features), bf16),
        in_specs=[SMEM, ANY] + [ANY] * 5,
        out_specs=VMEM,
        scratch_shapes=[
            pltpu.VMEM(branch.shape, bf16),
            pltpu.VMEM((2, 4, 4, features // 32, width), bf16),
            pltpu.SemaphoreType.DMA((11,)),
        ],
        name="project",
        compiler_params=pltpu.CompilerParams(vmem_limit_bytes=16 << 20),
    )(place, branch, *pieces)


def norm_rows(parts_hbm, residual_ref, gain_ref, parts_ref, sem):
    copy = pltpu.make_async_copy(parts_hbm, parts_ref, sem.at[0])
    copy.start()
    total = residual_scale * residual_ref[...].astype(f32)
    copy.wait()
    for x in range(parts_ref.shape[0]):
        total = total + parts_ref[x].astype(f32)
    center = total - jnp.mean(total, axis=-1, keepdims=True)
    variance = jnp.mean(center * center, axis=-1, keepdims=True)
    return (center * lax.rsqrt(variance + 1e-05) * gain_ref[...]).astype(bf16)


def norm_kernel(parts_hbm, residual_ref, gain_ref, out_ref, parts_ref, sem):
    out_ref[...] = norm_rows(parts_hbm, residual_ref, gain_ref, parts_ref, sem)


def copies_kernel(parts_hbm, residual_ref, gain_ref, out_ref, copies_ref, parts_ref, sem):
    out = norm_rows(parts_hbm, residual_ref, gain_ref, parts_ref, sem)
    out_ref[...] = out
    for x in range(copies_ref.shape[0]):
        copies_ref[x] = out


def norm(parts, residual, gain, copied):
    own = jax.ShapeDtypeStruct(residual.shape, bf16)
    copies = jax.ShapeDtypeStruct(parts.shape, bf16)
    return pl.pallas_call(
        copies_kernel if copied else norm_kernel,
        out_shape=(own, copies) if copied else own,
        in_specs=[ANY, VMEM, VMEM],
        out_specs=(VMEM, VMEM) if copied else VMEM,
        scratch_shapes=[pltpu.VMEM(parts.shape, bf16), pltpu.SemaphoreType.DMA((1,))],
        name="norm",
        compiler_params=pltpu.CompilerParams(vmem_limit_bytes=12 << 20),
    )(parts, residual, gain.reshape(1, -1))


def stage_kernel(place_ref, fed_hbm, gate_ref, up_ref, down_ref, sems):
    y = place_ref[1]
    height = gate_ref.shape[2]
    copies = []
    for at, away in enumerate((0, 3, 1, 2)):
        there = lax.rem(y + away, 4)
        for source, target in (
            (fed_hbm.at[0, :, at, :height], gate_ref.at[:, there]),
            (fed_hbm.at[1, :, at, :height], up_ref.at[:, there]),
            (fed_hbm.at[0, :, at, height:], down_ref.at[:, there, 0]),
            (fed_hbm.at[1, :, at, height:], down_ref.at[:, there, 1]),
        ):
            copies.append(pltpu.make_async_copy(source, target, sems.at[len(copies)]))
    start_all(copies)
    wait_all(copies)


def stage(place, fed):
    units = fed.shape[-1]
    height = fed.shape[3] * 2 // 3
    wide = jax.ShapeDtypeStruct((8, 4, height, units), bf16)
    down = jax.ShapeDtypeStruct((8, 4, 2, height // 2, units), bf16)
    return pl.pallas_call(
        stage_kernel,
        out_shape=(wide, wide, down),
        in_specs=[SMEM, HBM],
        out_specs=(VMEM, VMEM, VMEM),
        scratch_shapes=[pltpu.SemaphoreType.DMA((16,))],
        name="stage",
        compiler_params=pltpu.CompilerParams(vmem_limit_bytes=46 << 20),
    )(place, fed)


def feed_kernel(rows_hbm, gate_ref, up_ref, down_ref, out_ref, rows_ref, sem):
    copy = pltpu.make_async_copy(rows_hbm, rows_ref, sem.at[0])
    copy.start()
    copy.wait()
    units = gate_ref.shape[-1]
    rows = rows_ref[...].reshape(-1, rows_ref.shape[-1])
    gate = jnp.dot(rows, gate_ref[...].reshape(-1, units), preferred_element_type=f32)
    up = jnp.dot(rows, up_ref[...].reshape(-1, units), preferred_element_type=f32)
    hidden = (jax.nn.silu(gate) * up).astype(bf16)
    out = last_dims(hidden, down_ref[...].reshape(-1, units))
    out_ref[...] = out.astype(bf16).reshape(out_ref.shape)


def feed(rows, gate, up, down):
    return pl.pallas_call(
        feed_kernel,
        out_shape=jax.ShapeDtypeStruct(rows.shape, bf16),
        in_specs=[ANY, VMEM, VMEM, VMEM],
        out_specs=VMEM,
        scratch_shapes=[pltpu.VMEM(rows.shape, bf16), pltpu.SemaphoreType.DMA((1,))],
        name="feed",
        compiler_params=pltpu.CompilerParams(vmem_limit_bytes=16 << 20),
    )(rows, gate, up, down)


def to_partner(value):
    return lax.ppermute(value, "c", [(0, 1), (1, 0)])


def sideways(value, by):
    return lax.ppermute(value, "y", [(i, (i + by) % 4) for i in range(4)])


def round_y(line):
    after, before = sideways(line, 1), sideways(line, -1)
    middle = line.shape[0] // 2
    far = sideways(after[:middle], 1), sideways(before[middle:], -1)
    return (line, after, before, *far)


def sum_at_owner(keep, send):
    both = (keep.astype(f32) + to_partner(send).astype(f32)).astype(bf16)
    return lax.all_to_all(both, "x", 0, 0, tiled=True)


def local(
    tokens,
    recurrence_branch_weight,
    gate_branch_weight,
    convolution_kernel,
    recurrence_gate_blockwise,
    input_gate_blockwise,
    channel_decay_param,
    token_decay_shift,
    recurrence_output_weight,
    first_norm_gain,
    feedforward_gate_weight,
    feedforward_up_weight,
    feedforward_down_weight,
    second_norm_gain,
):
    length = tokens.shape[0]
    share = length // 8
    r = lax.axis_index("r")
    x, c = lax.axis_index("x"), lax.axis_index("c")
    y = lax.axis_index("y")
    place = jnp.stack([c, y]).astype(jnp.int32)
    partner = jnp.stack([1 - c, y]).astype(jnp.int32)
    channels = recurrence_branch_weight.shape[1]

    own_tokens = lax.dynamic_slice_in_dim(tokens, (2 * x + c) * share, share, 0)

    down = feedforward_down_weight.T
    height = down.shape[0]
    fed = jnp.concatenate(
        [
            jnp.where(r == 0, feedforward_gate_weight, feedforward_up_weight),
            jnp.where(r == 0, down[: height // 2], down[height // 2 :]),
        ],
        axis=0,
    )
    fed = lax.optimization_barrier(fed)
    moved = [sideways(fed, by) for by in (1, -1, 2)]
    fed_column = jnp.stack([fed, *moved])
    fed_all = lax.all_gather(fed_column, AROUND, axis=0, tiled=False)
    fed_all = fed_all.reshape(2, 8, 4, *fed.shape)

    first = jnp.concatenate(
        [recurrence_branch_weight, gate_branch_weight, recurrence_output_weight.T], axis=1
    )
    across = lax.ppermute(first, "zh", [(0, 1), (1, 0)])
    low = lax.axis_index("zh") == 0
    pair = jnp.stack([jnp.where(low, first, across), jnp.where(low, across, first)])
    line = copy_for_each(pair, "zl")
    branch_weight = round_y(line[..., : 2 * channels])
    output_weight = round_y(line[..., 2 * channels :])

    branch = mix(
        place,
        tokens,
        branch_weight,
        convolution_kernel,
        recurrence_gate_blockwise[0],
        input_gate_blockwise[0],
        channel_decay_param,
        token_decay_shift,
    )
    send = project(partner, branch, output_weight, share)
    mixed = sum_at_owner(project(place, branch, output_weight, share), send)
    normed, copies = norm(mixed, own_tokens, first_norm_gain, True)
    mine = lax.all_to_all(copies, "x", 0, 0, tiled=True)
    other = to_partner(mine)
    staged = stage(place, fed_all)
    keep = feed(mine, *staged)
    ffn = sum_at_owner(keep, feed(other, *staged))
    return norm(ffn, normed, second_norm_gain, False)


def solution(mesh):
    fine = Mesh(mesh.devices.reshape(2, 2, 4, 4, 4, 2), ("r", "zh", "zl", "y", "x", "c"))
    fs = ("zh", "zl", "y")
    tp = ("x", "c")
    return jax.shard_map(
        local,
        mesh=fine,
        in_specs=(
            P(("r", *fs), None),
            P(fs, tp),
            P(fs, tp),
            P(None, tp),
            P(tp, None, None),
            P(tp, None, None),
            P(tp),
            P(("r", *fs), tp),
            P(tp, fs),
            P(),
            P(fs, tp),
            P(fs, tp),
            P(tp, fs),
            P(),
        ),
        out_specs=P(("r", *fs, *tp), None),
        check_vma=False,
    )
```
